32 devices in a mesh: sp: 8 (over z, core), tp: 4 (over y, x).
Axes of the slice: x: 2, y: 2, z: 4, core: 2. Of those that a mesh axis runs over, the one named last changes fastest.
Arguments:
- residual_in: bfloat16 [2048, 2048], P(('sp', 'tp')), may hold values from -6 to 6
- query_a: bfloat16 [2048, 1024], P('sp', 'tp'), may hold values from -12 to 12
- key_a: bfloat16 [2048, 1024], P('sp', 'tp'), may hold values from -12 to 12
- value_a: bfloat16 [2048, 1024], P('sp', 'tp'), may hold values from -6 to 6
- query_b: bfloat16 [2048, 2048], P('sp', 'tp'), may hold values from -12 to 12
- key_b: bfloat16 [2048, 2048], P('sp', 'tp'), may hold values from -12 to 12
- value_b: bfloat16 [2048, 2048], P('sp', 'tp'), may hold values from -6 to 6
- cum_gates: float32 [2048, 2, 16], P('sp', None, 'tp'), may hold values from -247.76 to 0, as said below
- out_a: bfloat16 [1024, 2048], P('tp'), may hold values from -0.1875 to 0.1875
- out_b: bfloat16 [2048, 2048], P('tp'), may hold values from -0.125 to 0.125
- post_gain: bfloat16 [2048], replicated, may hold values from 0.099609375 to 1.8984375
- pre_gain: bfloat16 [2048], replicated, may hold values from 0.099609375 to 1.8984375
- expert_ids: int32 [2048, 2], P('sp'), may hold values from 0 to 7, all different within a row; in each aligned block of 256 rows (0 to 255, 256 to 511, ...) at most 80 rows name the same one
- expert_weights: float32 [2048, 2], P('sp'), may hold values from 0.2 to 1
- w_gate: bfloat16 [8, 2048, 4096], P('sp', None, 'tp'), may hold values from -0.125 to 0.125
- w_up: bfloat16 [8, 2048, 4096], P('sp', None, 'tp'), may hold values from -0.125 to 0.125
- w_down: bfloat16 [8, 4096, 2048], P('sp', 'tp'), may hold values from -0.09375 to 0.09375
Outputs:
- layer_out: bfloat16 [2048, 2048], P(('sp', 'tp'))
The draws below stay inside these ranges and needn't reach their ends.
Inputs may be any that keep to these rules, and one draw needn't show every extreme that they name: `expert_ids`: in each aligned block of 256 positions no expert is named by more than 80 routes, a bound that some block reaches; a token's experts differ. `cum_gates`: never rises along the positions.
All inputs are finite; a program needn't handle non-finite values.
Results may differ from the reference program's by a relative error of at most 0.015.
Values may be sent and summed in bfloat16 or wider, within the bound.
A program may use at most 64 MiB of HBM per device.

```python
import math
import jax
import jax.numpy as jnp
import numpy as np
from jax import lax

D = 2048
HEADS = 16
DA = 64
DB = 128
FF = 4096
TOP = 2
TOK_DEV = 256
SEQUENCE_TOKENS = 2048
EXPERTS = 8
FF_DEV = 1024
SLOTS = 80
N_SP = 8
N_TP = 4


def paired_rows(key, width):
    query_key, keys_key = jax.random.split(key, 2)
    shape = (SEQUENCE_TOKENS, HEADS * width)
    query = jnp.clip(jax.random.normal(query_key, shape, jnp.float32), -4.0, 4.0)
    key_rows = jnp.clip(jax.random.normal(keys_key, shape, jnp.float32), -4.0, 4.0)
    return (query, key_rows)


def value_matrix(key, width):
    noise_key, offset_key = jax.random.split(key, 2)
    shape = (SEQUENCE_TOKENS, HEADS * width)
    noise = jnp.clip(jax.random.normal(noise_key, shape, jnp.float32), -4.0, 4.0) * 0.7
    offsets = jnp.clip(jax.random.normal(offset_key, (N_SP, HEADS * width), jnp.float32), -3.0, 3.0)
    return noise + jnp.repeat(offsets, TOK_DEV, axis=0)


def draw_query_a(key, part):
    return paired_rows(jax.random.fold_in(key, 101), DA)[0].astype(jnp.bfloat16)


def draw_key_a(key, part):
    return paired_rows(jax.random.fold_in(key, 101), DA)[1].astype(jnp.bfloat16)


def draw_query_b(key, part):
    return paired_rows(jax.random.fold_in(key, 202), DB)[0].astype(jnp.bfloat16)


def draw_key_b(key, part):
    return paired_rows(jax.random.fold_in(key, 202), DB)[1].astype(jnp.bfloat16)


def draw_value_a(key, part):
    return value_matrix(jax.random.fold_in(key, 303), DA).astype(jnp.bfloat16)


def draw_value_b(key, part):
    return value_matrix(jax.random.fold_in(key, 404), DB).astype(jnp.bfloat16)


def draw_cum_gates(key, part):
    item_count = 2 * HEADS
    key_rows = jax.random.split(jax.random.fold_in(key, 505), 7)
    fast = jax.random.permutation(key_rows[0], item_count) < HEADS
    fast_span = jnp.exp(jax.random.uniform(key_rows[1], (item_count,), jnp.float32, math.log(30.0), math.log(100.0)))
    slow_total = jax.random.uniform(key_rows[2], (item_count,), jnp.float32, 0.4, 0.8)
    rate = jnp.where(fast, 1.0 / fast_span, slow_total / SEQUENCE_TOKENS)
    factor = jnp.exp(jax.random.uniform(key_rows[3], (N_SP,), jnp.float32, math.log(0.5), math.log(2.0)))
    rough = jax.random.uniform(key_rows[4], (SEQUENCE_TOKENS, item_count), jnp.float32, 0.3, 1.7)
    step_total = -rate[None, :] * jnp.repeat(factor, TOK_DEV)[:, None] * rough
    spike_position = jax.random.randint(key_rows[5], (2,), 0, SEQUENCE_TOKENS)
    spike_length = jnp.log(jax.random.uniform(key_rows[6], (2, item_count), jnp.float32, 0.5, 0.8))
    step_total = step_total.at[spike_position].add(spike_length)
    return jnp.cumsum(step_total, axis=0).reshape(SEQUENCE_TOKENS, 2, HEADS)


def levels(rng, extent, cuts, low, largest):
    level, own = 1.0, jax.random.fold_in(rng, 6)
    for dim, blocks in cuts:
        draws = jnp.exp(jax.random.uniform(jax.random.fold_in(own, dim), (blocks,), jnp.float32, low / len(cuts), largest / len(cuts)))
        level = level * jnp.repeat(draws, extent[dim] // blocks).reshape([-1 if axis == dim else 1 for axis in range(len(extent))])
    return level


def deal_out(own_key, own, number, rows, number_of, top, most, lean):
    ranking = jax.random.permutation(own_key, number_of)
    packed, common = portions_of(number_of, rows * top, most, lean, True), portions_of(number_of, rows * top, most, lean, False)
    places = jnp.arange(number_of)

    def named(sizes, rotation):
        used = int((sizes > 0).sum())
        fixed = max(1, used // 4)
        shifted = fixed + (places - fixed + rotation * (used - fixed)) % max(1, number_of - fixed)
        return jnp.zeros((number_of,), jnp.int32).at[ranking[jnp.where(places < fixed, places, shifted)]].set(jnp.asarray(sizes, jnp.int32))

    sizes = jnp.where(number % 4 == 0, named(packed, number // 4), named(common, number - number // 4 - 1))
    mixed = jax.random.permutation(jax.random.fold_in(own, 3), number_of)
    giver, receiver = mixed[0:number_of // 2 * 2:2], mixed[1:number_of // 2 * 2:2]
    slack = jnp.minimum(sizes[giver] - 1, most - sizes[receiver]) // 2
    slack = jnp.where((giver == ranking[0]) | (receiver == ranking[0]) | (sizes[receiver] == 0), 0, jnp.maximum(slack, 0))
    shifted = jax.random.randint(jax.random.fold_in(own, 4), (number_of // 2,), 0, 1 << 20) % (slack + 1)
    sizes = sizes.at[giver].add(-shifted).at[receiver].add(shifted)
    labels = jnp.searchsorted(jnp.cumsum(sizes), jnp.arange(rows * top), side="right").astype(jnp.int32)
    grid = labels.reshape(top, rows).T
    grid = grid[jax.random.permutation(jax.random.fold_in(own, 1), rows)]
    rotation = jax.random.randint(jax.random.fold_in(own, 2), (rows, 1), 0, top)
    return jnp.take_along_axis(grid, (jnp.arange(top)[None, :] + rotation) % top, axis=1)


def portions_of(count, total, most, skew, full):
    weights = [(1 << 20) // math.isqrt(standing ** skew) + 1 for standing in range(1, count + 1)]
    largest = most if full else min(most, max(-(-total // count), total * weights[0] // sum(weights)))
    least = 1 if total - largest >= count - 1 else 0
    holding, rest = [largest] + [least] * (count - 1), total - largest - least * (count - 1)
    while rest > 0:
        free = [i for i in range(1, count) if holding[i] < largest] or [i for i in range(1, count) if holding[i] < most]
        whole, remaining = sum([weights[i] for i in free]), rest
        for i in free:
            addition = min(most - holding[i], max(1, remaining * weights[i] // whole), rest)
            holding[i] = holding[i] + addition
            rest = rest - addition
    return np.array(holding)


def normal_values(own_key, shape, spread, reach, cuts=(), kind=jnp.bfloat16):
    values = spread * jax.random.normal(own_key, shape, jnp.float32)
    if cuts:
        values = values * levels(own_key, shape, cuts, -0.22, 0.18)
    return jnp.clip(values, -reach, reach).astype(kind)


def setup_inputs(seed: int = 0) -> dict:
    seeds = jax.random.split(jax.random.key(seed), 18)
    residual_in = normal_values(seeds[0], (SEQUENCE_TOKENS, D), 1.0, 6.0, ((0, 32),))
    query_a = draw_query_a(jax.random.fold_in(seeds[17], 71), 0)
    key_a = draw_key_a(jax.random.fold_in(seeds[17], 71), 0)
    value_a = draw_value_a(jax.random.fold_in(seeds[17], 71), 0)
    query_b = draw_query_b(jax.random.fold_in(seeds[17], 71), 0)
    key_b = draw_key_b(jax.random.fold_in(seeds[17], 71), 0)
    value_b = draw_value_b(jax.random.fold_in(seeds[17], 71), 0)
    cum_gates = draw_cum_gates(jax.random.fold_in(seeds[17], 71), 0)
    out_a = normal_values(seeds[8], (HEADS * DA, D), (HEADS * DA) ** -0.5, 0.1875, ((0, 4),))
    out_b = normal_values(seeds[9], (HEADS * DB, D), (HEADS * DB) ** -0.5, 0.125, ((0, 4),))
    post_gain = jnp.clip(1.0 + 0.18 * jax.random.normal(seeds[10], (D,), jnp.float32), 0.099609375, 1.8984375).astype(jnp.bfloat16)
    pre_gain = jnp.clip(1.0 + 0.18 * jax.random.normal(seeds[11], (D,), jnp.float32), 0.099609375, 1.8984375).astype(jnp.bfloat16)
    expert_ids_keys = jax.random.split(jax.random.fold_in(seeds[12], 1), SEQUENCE_TOKENS // TOK_DEV)
    expert_ids_turns = jax.random.permutation(jax.random.fold_in(seeds[12], 3), SEQUENCE_TOKENS // TOK_DEV)
    expert_ids = jax.vmap(lambda own, number: deal_out(jax.random.fold_in(seeds[12], 2), own, number, TOK_DEV, EXPERTS, TOP, SLOTS, 2))(expert_ids_keys, expert_ids_turns).reshape((SEQUENCE_TOKENS, TOP))
    expert_weights = jnp.clip(jnp.exp(math.log(1.0) - 1.609438 * jax.random.uniform(seeds[13], (SEQUENCE_TOKENS, TOP), jnp.float32) ** levels(seeds[13], (SEQUENCE_TOKENS, TOP), ((0, 8),), -0.2, 0.2)), 0.2, 1.0)
    w_gate = normal_values(seeds[14], (EXPERTS, D, FF), D ** -0.5, 0.125, ((0, 8), (2, 4)))
    w_up = normal_values(seeds[15], (EXPERTS, D, FF), D ** -0.5, 0.125, ((0, 8), (2, 4)))
    w_down = normal_values(seeds[16], (EXPERTS, FF, D), FF ** -0.5, 0.09375, ((0, 8), (1, 4)))
    return dict(residual_in=residual_in, query_a=query_a, key_a=key_a, value_a=value_a, query_b=query_b, key_b=key_b, value_b=value_b, cum_gates=cum_gates, out_a=out_a, out_b=out_b, post_gain=post_gain, pre_gain=pre_gain, expert_ids=expert_ids, expert_weights=expert_weights, w_gate=w_gate, w_up=w_up, w_down=w_down)


eps_norm = 1e-06
big_neg = -1e+30

def group_attention(query, key_rows, values, gates, width):
    total_rows = query.shape[0]
    heads = gates.shape[1]
    query_heads = query.reshape(total_rows, heads, width).transpose(1, 0, 2)
    key_heads = key_rows.reshape(total_rows, heads, width).transpose(1, 0, 2)
    value_heads = values.reshape(total_rows, heads, width).transpose(1, 0, 2)
    gate_heads = gates.T
    block = min(512, total_rows)
    blocks = total_rows // block
    key_pos = jnp.arange(total_rows, dtype=jnp.int32)

    def one_head(pieces):
        head_query, head_key, head_value, head_gate = pieces

        def one_block(index):
            start = (index * block).astype(jnp.int32)
            block_query = lax.dynamic_slice_in_dim(head_query, start, block, 0)
            block_gate = lax.dynamic_slice_in_dim(head_gate, start, block, 0)
            score = jnp.dot(block_query, head_key.T, preferred_element_type=jnp.float32) * width ** (-0.5)
            score = score + block_gate[:, None] - head_gate[None, :]
            position = start + jnp.arange(block, dtype=jnp.int32)
            mask = key_pos[None, :] <= position[:, None]
            highest = lax.optimization_barrier(jnp.max(jnp.where(mask, score, big_neg), axis=1, keepdims=True))
            expo = jnp.exp(jnp.where(mask, score - highest, big_neg))
            total = lax.optimization_barrier(jnp.sum(expo, axis=1, keepdims=True))
            mixed = jnp.dot(expo.astype(jnp.bfloat16), head_value, preferred_element_type=jnp.float32)
            return (mixed / total).astype(jnp.bfloat16)
        return lax.map(one_block, jnp.arange(blocks, dtype=jnp.int32)).reshape(total_rows, width)
    result = lax.map(one_head, (query_heads, key_heads, value_heads, gate_heads))
    return result.transpose(1, 0, 2).reshape(total_rows, heads * width)

def head_projection(attn_a, attn_b, out_a, out_b):
    rows_a = out_a.shape[0] // N_TP
    rows_b = out_b.shape[0] // N_TP

    def add_block(index, accum):
        part_a = lax.dynamic_slice_in_dim(attn_a, index * rows_a, rows_a, 1)
        weight_a = lax.dynamic_slice_in_dim(out_a, index * rows_a, rows_a, 0)
        part_b = lax.dynamic_slice_in_dim(attn_b, index * rows_b, rows_b, 1)
        weight_b = lax.dynamic_slice_in_dim(out_b, index * rows_b, rows_b, 0)
        term = jnp.dot(part_a, weight_a, preferred_element_type=jnp.float32) + jnp.dot(part_b, weight_b, preferred_element_type=jnp.float32)
        rounded = lax.optimization_barrier(term.astype(jnp.bfloat16))
        return accum + rounded.astype(jnp.float32)
    start = jnp.zeros((attn_a.shape[0], out_a.shape[1]), jnp.float32)
    return lax.fori_loop(0, N_TP, add_block, start).astype(jnp.bfloat16)

def rms_scale(values, gain):
    return values * lax.rsqrt(lax.optimization_barrier(jnp.mean(values * values, axis=-1, keepdims=True)) + eps_norm) * gain

def reference(residual_in, query_a, key_a, value_a, query_b, key_b, value_b, cum_gates, out_a, out_b, post_gain, pre_gain, expert_ids, expert_weights, w_gate, w_up, w_down):
    attn_a = group_attention(query_a, key_a, value_a, cum_gates[:, 0, :], DA)
    attn_b = group_attention(query_b, key_b, value_b, cum_gates[:, 1, :], DB)
    proj = head_projection(attn_a, attn_b, out_a, out_b)
    post = rms_scale(proj.astype(jnp.float32), post_gain.astype(jnp.float32))
    mid_stream = (residual_in.astype(jnp.float32) + post).astype(jnp.bfloat16)
    normed = rms_scale(mid_stream.astype(jnp.float32), pre_gain.astype(jnp.float32)).astype(jnp.bfloat16)
    block_ids = expert_ids.reshape(N_SP, TOK_DEV * TOP)
    onehot = (block_ids[:, :, None] == jnp.arange(EXPERTS, dtype=jnp.int32)[None, None, :]).astype(jnp.int32)
    rank = lax.optimization_barrier(jnp.sum((jnp.cumsum(onehot, axis=1) - onehot) * onehot, axis=2))
    block_index = jnp.arange(N_SP, dtype=jnp.int32)[:, None]
    target = block_ids * (N_SP * SLOTS) + block_index * SLOTS + rank
    owner = block_index * TOK_DEV + jnp.arange(TOK_DEV * TOP, dtype=jnp.int32)[None, :] // TOP
    table = jnp.full((EXPERTS * N_SP * SLOTS,), -1, jnp.int32).at[target.reshape(-1)].set(owner.reshape(-1))
    table = table.reshape(EXPERTS, N_SP * SLOTS)

    def run_expert(pieces):
        row_index, gate_weight, up_weight, down_weight = pieces
        live = row_index >= 0
        rows = jnp.where(live[:, None], normed[jnp.maximum(row_index, 0)], jnp.zeros((), jnp.bfloat16))
        gate = jnp.dot(rows, gate_weight, preferred_element_type=jnp.float32)
        upward = jnp.dot(rows, up_weight, preferred_element_type=jnp.float32)
        hidden = (jax.nn.silu(gate) * upward).astype(jnp.bfloat16)
        parts = jnp.einsum('rjf,jfd->rjd', hidden.reshape(-1, N_TP, FF_DEV).astype(jnp.float32), down_weight.reshape(N_TP, FF_DEV, D).astype(jnp.float32))
        rounded = lax.optimization_barrier(parts.astype(jnp.bfloat16))
        return lax.optimization_barrier(jnp.sum(rounded.astype(jnp.float32), axis=1)).astype(jnp.bfloat16)
    expert_out = lax.map(run_expert, (table, w_gate, w_up, w_down))
    slot_of = rank.reshape(SEQUENCE_TOKENS, TOP)
    token_block = (jnp.arange(SEQUENCE_TOKENS, dtype=jnp.int32) // TOK_DEV)[:, None]
    picked = expert_out[expert_ids, token_block * SLOTS + slot_of]
    mixture = lax.optimization_barrier(jnp.sum(expert_weights[:, :, None] * picked.astype(jnp.float32), axis=1))
    return (mid_stream.astype(jnp.float32) + mixture).astype(jnp.bfloat16)
```

```python
import functools

import jax
import jax.numpy as jnp
from jax import lax
from jax.experimental import pallas as pl
from jax.experimental.pallas import tpu as pltpu
from jax.sharding import PartitionSpec as P

eps_norm = 1e-06
big_neg = -1e30


def rms_scale(values, gain):
    return values * lax.rsqrt(jnp.mean(values * values, axis=-1, keepdims=True) + eps_norm) * gain


def empty_state(item_count, heads, width):
    return (
        jnp.full((heads, item_count), big_neg, jnp.float32),
        jnp.zeros((heads, item_count), jnp.float32),
        jnp.zeros((heads, item_count, width), jnp.float32),
    )


def update_state(state, query, key_rows, values, query_gate, key_gate, mask, width):
    highest, total, accum = state
    score = jnp.einsum(
        "rhd,khd->hrk", query, key_rows, preferred_element_type=jnp.float32
    ) * width ** (-0.5)
    score = score + query_gate.T[:, :, None] - key_gate.T[:, None, :]
    new_high = jnp.maximum(highest, jnp.max(jnp.where(mask[None], score, big_neg), axis=2))
    expo = jnp.exp(jnp.where(mask[None], score - new_high[:, :, None], big_neg))
    total = jnp.sum(expo, axis=2)
    accum = jnp.einsum(
        "hrk,khd->hrd", expo.astype(jnp.bfloat16), values, preferred_element_type=jnp.float32
    )
    return (new_high, total, accum)


def finish(state):
    highest, total, accum = state
    heads, item_count, width = accum.shape
    result = accum / total[:, :, None]
    return result.transpose(1, 0, 2).reshape(item_count, heads * width).astype(jnp.bfloat16)


def exchange_kernel(axis, count, plans, *refs):
    arrays = len(plans)
    ins, outs = refs[:arrays], refs[arrays : 2 * arrays]
    send_sem, recv_sem, own_sem = refs[2 * arrays :]
    me = lax.axis_index(axis)

    barrier = pltpu.get_barrier_semaphore()
    for step in range(1, count):
        pl.semaphore_signal(
            barrier,
            inc=1,
            device_id={axis: lax.rem(me + step, count)},
            device_id_type=pl.DeviceIdType.MESH,
        )
    pl.semaphore_wait(barrier, count - 1)

    def remote(index, step, peer, sender):
        source, target, _ = plans[index]
        return pltpu.make_async_remote_copy(
            src_ref=source(ins[index], peer),
            dst_ref=target(outs[index], sender),
            send_sem=send_sem.at[index, step],
            recv_sem=recv_sem.at[index, step],
            device_id={axis: peer},
            device_id_type=pl.DeviceIdType.MESH,
        )

    def own(index):
        source, target, _ = plans[index]
        return pltpu.make_async_copy(
            source(ins[index], me), target(outs[index], me), own_sem.at[index]
        )

    def guarded(least, who, action):
        if least:
            pl.when(who >= least)(action)
        else:
            action()

    for step in range(1, count):
        peer = lax.rem(me + step, count)
        for index in range(arrays):
            guarded(
                plans[index][2], peer, lambda: remote(index, step, peer, me).start()
            )
    for index in range(arrays):
        guarded(plans[index][2], me, lambda: own(index).start())
    for index in range(arrays):
        guarded(plans[index][2], me, lambda: own(index).wait())
    for step in range(1, count):
        peer = lax.rem(me + step, count)
        sender = lax.rem(me + count - step, count)
        for index in range(arrays):
            guarded(
                plans[index][2], me, lambda: remote(index, step, peer, sender).wait_recv()
            )
            guarded(
                plans[index][2], peer, lambda: remote(index, step, peer, me).wait_send()
            )


def exchange(values, shapes, plans, axis, name):
    count = lax.axis_size(axis)
    arrays = len(values)
    result = pl.pallas_call(
        functools.partial(exchange_kernel, axis, count, plans),
        out_shape=[
            jax.ShapeDtypeStruct(shape, value.dtype) for shape, value in zip(shapes, values)
        ],
        in_specs=[pl.BlockSpec(memory_space=pltpu.VMEM)] * arrays,
        out_specs=[pl.BlockSpec(memory_space=pltpu.VMEM)] * arrays,
        scratch_shapes=[
            pltpu.SemaphoreType.DMA((arrays, count)),
            pltpu.SemaphoreType.DMA((arrays, count)),
            pltpu.SemaphoreType.DMA((arrays,)),
        ],
        compiler_params=pltpu.CompilerParams(collective_id=name, has_side_effects=True),
    )(*values)
    return result


def item(ref, index):
    return ref.at[index]


def whole_ref(ref, index):
    return ref


def column_block(width):
    return lambda ref, index: ref.at[:, pl.ds(pl.multiple_of(index * width, width), width)]


def row_block(height):
    return lambda ref, index: ref.at[pl.ds(pl.multiple_of(index * height, height), height), :]


def attend_kernel(block, scale_ref, query_ref, key_ref, value_ref, row_ref, col_ref, out_ref):
    scale = scale_ref[0]
    total_rows = query_ref.shape[0]
    lower = lax.broadcasted_iota(jnp.int32, (block, block), 1) <= lax.broadcasted_iota(
        jnp.int32, (block, block), 0
    )
    dims = (((1,), (1,)), ((), ()))
    for start in range(0, total_rows, block):
        here = slice(start, start + block)
        query = query_ref[here, :]
        gate = col_ref[here, :]
        diag = lax.dot_general(query, key_ref[here, :], dims, preferred_element_type=jnp.float32)
        diag = diag * scale + gate - row_ref[0:1, here]
        diag = jnp.where(lower, diag, big_neg)
        highest = jnp.max(diag, axis=1, keepdims=True)
        if start:
            early = slice(0, start)
            score = lax.dot_general(
                query, key_ref[early, :], dims, preferred_element_type=jnp.float32
            )
            score = score * scale + gate - row_ref[0:1, early]
            highest = jnp.maximum(highest, jnp.max(score, axis=1, keepdims=True))
        expo = jnp.exp(diag - highest)
        total = jnp.sum(expo, axis=1, keepdims=True)
        mixed = jnp.dot(
            expo.astype(jnp.bfloat16), value_ref[here, :], preferred_element_type=jnp.float32
        )
        if start:
            expo = jnp.exp(score - highest)
            total = total + jnp.sum(expo, axis=1, keepdims=True)
            mixed = mixed + jnp.dot(
                expo.astype(jnp.bfloat16), value_ref[early, :], preferred_element_type=jnp.float32
            )
        out_ref[here, :] = (mixed / total).astype(jnp.bfloat16)


def headwise_attention(
    query_a, key_a, value_a, query_b, key_b, value_b, cum_gates
):
    rows = query_a.shape[0]
    heads = cum_gates.shape[2]
    width_a = query_a.shape[1] // heads
    width_b = query_b.shape[1] // heads
    count = lax.axis_size("sp")
    me = lax.axis_index("sp")

    def split(values, width):
        return values.reshape(rows, heads, width).transpose(1, 0, 2)

    pad = jnp.zeros((heads, rows, 2 * width_b - 3 * width_a), jnp.bfloat16)
    first = jnp.concatenate(
        [split(query_a, width_a), split(key_a, width_a), split(value_a, width_a), pad], axis=2
    )
    second = jnp.concatenate([split(query_b, width_b), split(key_b, width_b)], axis=2)
    packed = jnp.concatenate([first, second], axis=0)
    late = split(value_b, width_b)
    gates = cum_gates.transpose(1, 2, 0).reshape(2 * heads, 1, rows)
    gates = jnp.broadcast_to(gates, (2 * heads, 8, rows))
    main, tail, gate_rows = exchange(
        [packed, late, gates],
        [
            (count * rows, 2 * width_b),
            (count * rows, width_b),
            (8, count * rows),
        ],
        [
            (item, row_block(rows), 0),
            (lambda ref, index: ref.at[jnp.maximum(index - heads, 0)], row_block(rows), heads),
            (item, column_block(rows), 0),
        ],
        "sp",
        1,
    )
    narrow_head = me < heads
    fill = jnp.zeros((count * rows, width_b - width_a), jnp.bfloat16)

    def widen(index):
        return jnp.concatenate([main[:, index * width_a : (index + 1) * width_a], fill], axis=1)

    query = jnp.where(narrow_head, widen(0), main[:, :width_b])
    keys = jnp.where(narrow_head, widen(1), main[:, width_b:])
    values = jnp.where(narrow_head, widen(2), tail)
    scale = jnp.where(narrow_head, width_a ** (-0.5), width_b ** (-0.5)).astype(jnp.float32)
    mixed = pl.pallas_call(
        functools.partial(attend_kernel, rows),
        out_shape=jax.ShapeDtypeStruct((count * rows, width_b), jnp.bfloat16),
        in_specs=[pl.BlockSpec(memory_space=pltpu.SMEM)]
        + [pl.BlockSpec(memory_space=pltpu.VMEM)] * 5,
        out_specs=pl.BlockSpec(memory_space=pltpu.VMEM),
    )(scale.reshape(1), query, keys, values, gate_rows, gate_rows[0].reshape(-1, 1))
    (back,) = exchange(
        [mixed], [(count, rows, width_b)], [(row_block(rows), item, 0)], "sp", 2
    )
    attn_a = back[:heads, :, :width_a].transpose(1, 0, 2).reshape(rows, heads * width_a)
    attn_b = back[heads:].transpose(1, 0, 2).reshape(rows, heads * width_b)
    return attn_a, attn_b


def gathered_attention(
    query_a, key_a, value_a, query_b, key_b, value_b, cum_gates
):
    rows = query_a.shape[0]
    heads = cum_gates.shape[2]
    width_a = query_a.shape[1] // heads
    width_b = query_b.shape[1] // heads
    here = lax.axis_index("sp")
    offset = here * rows
    gates_all = lax.all_gather(cum_gates, "sp", axis=0, tiled=True)
    queries_a = query_a.reshape(rows, heads, width_a)
    queries_b = query_b.reshape(rows, heads, width_b)
    blocks = [(queries_a, queries_b, offset + jnp.arange(rows, dtype=jnp.int32), cum_gates)]
    initial = tuple(
        (
            (
                empty_state(block[2].shape[0], heads, width_a),
                empty_state(block[2].shape[0], heads, width_b),
            )
            for block in blocks
        )
    )
    start = jnp.int32(0)
    piece_key_a = lax.all_gather(key_a.reshape(rows, heads, width_a), "sp", axis=0, tiled=True)
    piece_value_a = lax.all_gather(value_a.reshape(rows, heads, width_a), "sp", axis=0, tiled=True)
    piece_key_b = lax.all_gather(key_b.reshape(rows, heads, width_b), "sp", axis=0, tiled=True)
    piece_value_b = lax.all_gather(value_b.reshape(rows, heads, width_b), "sp", axis=0, tiled=True)
    item_count = piece_key_a.shape[0]
    key_pos = jnp.arange(item_count, dtype=jnp.int32)
    updated = []
    for state, (block_a, block_b, position, block_gate) in zip(initial, blocks):

        def compute(current):
            mask = key_pos[None, :] <= position[:, None]
            return (
                update_state(
                    current[0],
                    block_a,
                    piece_key_a,
                    piece_value_a,
                    block_gate[:, 0, :],
                    gates_all[:, 0, :],
                    mask,
                    width_a,
                ),
                update_state(
                    current[1],
                    block_b,
                    piece_key_b,
                    piece_value_b,
                    block_gate[:, 1, :],
                    gates_all[:, 1, :],
                    mask,
                    width_b,
                ),
            )

        updated.append(lax.cond(start <= position[-1], compute, lambda current: current, state))
    folded = tuple(updated)
    attn_a = finish(folded[0][0])
    attn_b = finish(folded[0][1])
    return attn_a, attn_b


def per_device(
    residual_in,
    query_a,
    key_a,
    value_a,
    query_b,
    key_b,
    value_b,
    cum_gates,
    out_a,
    out_b,
    post_gain,
    pre_gain,
    expert_ids,
    expert_weights,
    w_gate,
    w_up,
    w_down,
):
    rows = query_a.shape[0]
    heads = cum_gates.shape[2]
    width_a = query_a.shape[1] // heads
    width_b = query_b.shape[1] // heads
    group_size = lax.axis_size("sp")
    narrow = lax.axis_size("tp")
    columns = out_a.shape[1] // narrow
    own_rows = rows // narrow
    fits = 2 * heads == group_size and 2 * width_b >= 3 * width_a and width_b >= width_a
    attention = headwise_attention if fits else gathered_attention
    attn_a, attn_b = attention(query_a, key_a, value_a, query_b, key_b, value_b, cum_gates)
    part = (
        jnp.dot(attn_a, out_a, preferred_element_type=jnp.float32)
        + jnp.dot(attn_b, out_b, preferred_element_type=jnp.float32)
    ).astype(jnp.bfloat16)
    (parts,) = exchange(
        [part],
        [(narrow, own_rows, part.shape[1])],
        [(row_block(own_rows), item, 0)],
        "tp",
        3,
    )
    proj = jnp.sum(parts.astype(jnp.float32), axis=0).astype(jnp.bfloat16)
    post = rms_scale(proj.astype(jnp.float32), post_gain.astype(jnp.float32))
    mid_stream = (residual_in.astype(jnp.float32) + post).astype(jnp.bfloat16)
    normed = rms_scale(mid_stream.astype(jnp.float32), pre_gain.astype(jnp.float32)).astype(
        jnp.bfloat16
    )
    selected_count = expert_ids.shape[1]
    slots = rows * selected_count * 5 // (4 * group_size)
    named = expert_ids[:, :, None] == jnp.arange(group_size, dtype=jnp.int32)
    position = jnp.arange(rows, dtype=jnp.int32)
    before = (position[None, :] < position[:, None]).astype(jnp.bfloat16)
    earlier = jnp.dot(
        before, jnp.any(named, axis=1).astype(jnp.bfloat16), preferred_element_type=jnp.float32
    ).astype(jnp.int32)
    rank = jnp.sum(jnp.where(named, earlier[:, None, :], 0), axis=2)
    target = expert_ids * slots + rank
    chosen = target[:, :, None] == jnp.arange(group_size * slots, dtype=jnp.int32)
    weighting = jnp.sum(jnp.where(chosen, expert_weights[:, :, None], 0.0), axis=1)
    placing = jnp.any(chosen, axis=1).astype(jnp.bfloat16)
    (column_rows,) = exchange(
        [normed],
        [(rows, columns)],
        [(column_block(columns), row_block(own_rows), 0)],
        "tp",
        4,
    )
    outgoing = lax.dot_general(
        placing, column_rows, (((0,), (0,)), ((), ())), preferred_element_type=jnp.float32
    ).astype(jnp.bfloat16)
    outgoing = outgoing.reshape(group_size, slots, columns)
    (arrived,) = exchange(
        [outgoing], [(group_size, slots, columns)], [(item, item, 0)], "sp", 5
    )
    (piece,) = exchange(
        [arrived.reshape(-1, columns)],
        [(group_size * slots, columns * narrow)],
        [(whole_ref, column_block(columns), 0)],
        "tp",
        6,
    )
    gate = jnp.dot(piece, w_gate[0], preferred_element_type=jnp.float32)
    upward = jnp.dot(piece, w_up[0], preferred_element_type=jnp.float32)
    hidden = (jax.nn.silu(gate) * upward).astype(jnp.bfloat16)
    down = jnp.dot(hidden, w_down[0], preferred_element_type=jnp.float32).astype(jnp.bfloat16)
    (downs,) = exchange(
        [down],
        [(narrow, group_size * slots, columns)],
        [(column_block(columns), item, 0)],
        "tp",
        7,
    )
    summed = jnp.sum(downs.astype(jnp.float32), axis=0).astype(jnp.bfloat16)
    (returned,) = exchange(
        [summed.reshape(group_size, slots, columns)],
        [(group_size, slots, columns)],
        [(item, item, 0)],
        "sp",
        8,
    )
    mixture_cols = jnp.dot(
        weighting,
        returned.reshape(group_size * slots, columns).astype(jnp.float32),
        precision=lax.Precision.HIGHEST,
    )
    (mixture,) = exchange(
        [mixture_cols.astype(jnp.bfloat16)],
        [(own_rows, columns * narrow)],
        [(row_block(own_rows), column_block(columns), 0)],
        "tp",
        9,
    )
    return (mid_stream.astype(jnp.float32) + mixture.astype(jnp.float32)).astype(jnp.bfloat16)


def solution(mesh):
    placed = (
        P(("sp", "tp"), None),
        P("sp", "tp"),
        P("sp", "tp"),
        P("sp", "tp"),
        P("sp", "tp"),
        P("sp", "tp"),
        P("sp", "tp"),
        P("sp", None, "tp"),
        P("tp", None),
        P("tp", None),
        P(),
        P(),
        P("sp", None),
        P("sp", None),
        P("sp", None, "tp"),
        P("sp", None, "tp"),
        P("sp", "tp", None),
    )
    return jax.shard_map(
        per_device, mesh=mesh, in_specs=placed, out_specs=P(("sp", "tp"), None), check_vma=False
    )
```

```python
import functools

import jax
import jax.numpy as jnp
from jax import lax
from jax.experimental import pallas as pl
from jax.experimental.pallas import tpu as pltpu
from jax.sharding import PartitionSpec as P

eps_norm = 1e-06
big_neg = -1e30


def rms_scale(values, gain):
    return values * lax.rsqrt(jnp.mean(values * values, axis=-1, keepdims=True) + eps_norm) * gain


def empty_state(item_count, heads, width):
    return (
        jnp.full((heads, item_count), big_neg, jnp.float32),
        jnp.zeros((heads, item_count), jnp.float32),
        jnp.zeros((heads, item_count, width), jnp.float32),
    )


def update_state(state, query, key_rows, values, query_gate, key_gate, mask, width):
    highest, total, accum = state
    score = jnp.einsum(
        "rhd,khd->hrk", query, key_rows, preferred_element_type=jnp.float32
    ) * width ** (-0.5)
    score = score + query_gate.T[:, :, None] - key_gate.T[:, None, :]
    new_high = jnp.maximum(highest, jnp.max(jnp.where(mask[None], score, big_neg), axis=2))
    expo = jnp.exp(jnp.where(mask[None], score - new_high[:, :, None], big_neg))
    total = jnp.sum(expo, axis=2)
    accum = jnp.einsum(
        "hrk,khd->hrd", expo.astype(jnp.bfloat16), values, preferred_element_type=jnp.float32
    )
    return (new_high, total, accum)


def finish(state):
    highest, total, accum = state
    heads, item_count, width = accum.shape
    result = accum / total[:, :, None]
    return result.transpose(1, 0, 2).reshape(item_count, heads * width).astype(jnp.bfloat16)


def exchange_kernel(axis, count, plans, *refs):
    arrays = len(plans)
    ins, outs = refs[:arrays], refs[arrays : 2 * arrays]
    send_sem, recv_sem, own_sem = refs[2 * arrays :]
    me = lax.axis_index(axis)

    barrier = pltpu.get_barrier_semaphore()
    for step in range(1, count):
        pl.semaphore_signal(
            barrier,
            inc=1,
            device_id={axis: lax.rem(me + step, count)},
            device_id_type=pl.DeviceIdType.MESH,
        )
    pl.semaphore_wait(barrier, count - 1)

    def remote(index, step, peer, sender):
        source, target, _ = plans[index]
        return pltpu.make_async_remote_copy(
            src_ref=source(ins[index], peer),
            dst_ref=target(outs[index], sender),
            send_sem=send_sem.at[index, step],
            recv_sem=recv_sem.at[index, step],
            device_id={axis: peer},
            device_id_type=pl.DeviceIdType.MESH,
        )

    def own(index):
        source, target, _ = plans[index]
        return pltpu.make_async_copy(
            source(ins[index], me), target(outs[index], me), own_sem.at[index]
        )

    def guarded(least, who, action):
        if least:
            pl.when(who >= least)(action)
        else:
            action()

    for step in range(1, count):
        peer = lax.rem(me + step, count)
        for index in range(arrays):
            guarded(
                plans[index][2], peer, lambda: remote(index, step, peer, me).start()
            )
    for index in range(arrays):
        guarded(plans[index][2], me, lambda: own(index).start())
    for index in range(arrays):
        guarded(plans[index][2], me, lambda: own(index).wait())
    for step in range(1, count):
        peer = lax.rem(me + step, count)
        sender = lax.rem(me + count - step, count)
        for index in range(arrays):
            guarded(
                plans[index][2], me, lambda: remote(index, step, peer, sender).wait_recv()
            )
            guarded(
                plans[index][2], peer, lambda: remote(index, step, peer, me).wait_send()
            )


def exchange(values, shapes, plans, axis, name):
    count = lax.axis_size(axis)
    arrays = len(values)
    result = pl.pallas_call(
        functools.partial(exchange_kernel, axis, count, plans),
        out_shape=[
            jax.ShapeDtypeStruct(shape, value.dtype) for shape, value in zip(shapes, values)
        ],
        in_specs=[pl.BlockSpec(memory_space=pltpu.VMEM)] * arrays,
        out_specs=[pl.BlockSpec(memory_space=pltpu.VMEM)] * arrays,
        scratch_shapes=[
            pltpu.SemaphoreType.DMA((arrays, count)),
            pltpu.SemaphoreType.DMA((arrays, count)),
            pltpu.SemaphoreType.DMA((arrays,)),
        ],
        compiler_params=pltpu.CompilerParams(collective_id=name, has_side_effects=True),
    )(*values)
    return result


def item(ref, index):
    return ref.at[index]


def whole_ref(ref, index):
    return ref


def column_block(width):
    return lambda ref, index: ref.at[:, pl.ds(pl.multiple_of(index * width, width), width)]


def row_block(height):
    return lambda ref, index: ref.at[pl.ds(pl.multiple_of(index * height, height), height), :]


def greet(axes):
    barrier = pltpu.get_barrier_semaphore()
    for axis, count in axes:
        me = lax.axis_index(axis)
        for step in range(1, count):
            pl.semaphore_signal(
                barrier,
                inc=1,
                device_id={axis: lax.rem(me + step, count)},
                device_id_type=pl.DeviceIdType.MESH,
            )
    pl.semaphore_wait(barrier, sum(count - 1 for _, count in axes))


def send(source, target, sent, landed, axis, peer):
    return pltpu.make_async_remote_copy(
        src_ref=source,
        dst_ref=target,
        send_sem=sent,
        recv_sem=landed,
        device_id={axis: peer},
        device_id_type=pl.DeviceIdType.MESH,
    )


def attend_block(block, index, width, starts, main, tail, gate_rows, mixed):
    query_at, key_at, value_at = starts
    scale = width ** (-0.5)
    start = index * block
    here = slice(start, start + block)
    early = slice(0, start)
    dims = (((1,), (1,)), ((), ()))

    def values(rows):
        if value_at is None:
            return tail[rows, :]
        return main[rows, value_at : value_at + width]

    gate = jnp.broadcast_to(gate_rows[0:1, here], (128, block)).T[:, 0:1]
    query = main[here, query_at : query_at + width]
    lower = lax.broadcasted_iota(jnp.int32, (block, block), 1) <= lax.broadcasted_iota(
        jnp.int32, (block, block), 0
    )

    def scores(rows):
        dot = lax.dot_general(
            query,
            main[rows, key_at : key_at + width],
            dims,
            preferred_element_type=jnp.float32,
        )
        return dot * scale + gate - gate_rows[0:1, rows]

    diag = jnp.where(lower, scores(here), big_neg)
    highest = jnp.max(diag, axis=1, keepdims=True)
    if start:
        score = scores(early)
        highest = jnp.maximum(highest, jnp.max(score, axis=1, keepdims=True))
    expo = jnp.exp(diag - highest)
    total = jnp.sum(expo, axis=1, keepdims=True)
    result = jnp.dot(expo.astype(jnp.bfloat16), values(here), preferred_element_type=jnp.float32)
    if start:
        expo = jnp.exp(score - highest)
        total = total + jnp.sum(expo, axis=1, keepdims=True)
        result = result + jnp.dot(
            expo.astype(jnp.bfloat16), values(early), preferred_element_type=jnp.float32
        )
    result = (result / total).astype(jnp.bfloat16)
    if result.shape[1] < mixed.shape[1]:
        fill = jnp.zeros((block, mixed.shape[1] - result.shape[1]), jnp.bfloat16)
        result = jnp.concatenate([result, fill], axis=1)
    mixed[here, :] = result


def attend_kernel(
    count, rows, width_a, width_b, packed, late, gates, back,
    main, tail, gate_rows, mixed, sent, landed, own_sem, back_sent, back_landed,
):
    me = lax.axis_index("sp")
    second = lax.rem(me, 2) == 1
    greet([("sp", count)])

    def rows_of(ref, index):
        return ref.at[pl.ds(pl.multiple_of(index * rows, rows), rows), :]

    def pieces(dest, sender):
        return (
            (packed.at[dest], rows_of(main, sender)),
            (gates.at[dest], gate_rows.at[:, pl.ds(pl.multiple_of(sender * rows, rows), rows)]),
            (late.at[dest // 2], rows_of(tail, sender)),
        )

    def remote(kind, step, dest, sender):
        source, target = pieces(dest, sender)[kind]
        return send(source, target, sent.at[kind, step], landed.at[kind, step], "sp", dest)

    def own(kind):
        source, target = pieces(me, me)[kind]
        return pltpu.make_async_copy(source, target, own_sem.at[kind])

    for step in range(1, count):
        dest = lax.rem(me + step, count)
        remote(0, step, dest, me).start()
        remote(1, step, dest, me).start()
        pl.when(lax.rem(dest, 2) == 1)(lambda: remote(2, step, dest, me).start())
    own(0).start()
    own(1).start()
    pl.when(second)(lambda: own(2).start())
    own(0).wait()
    own(1).wait()
    pl.when(second)(lambda: own(2).wait())

    def back_copy(dest, sender):
        return send(
            rows_of(mixed, dest), back.at[sender], back_sent.at[dest], back_landed.at[sender],
            "sp", dest,
        )

    def back_own():
        return pltpu.make_async_copy(rows_of(mixed, me), back.at[me], back_sent.at[me])

    for index in range(count):

        @pl.when(me != index)
        def _():
            step = lax.rem(me - index + count, count)
            remote(0, step, me, index).wait_recv()
            remote(1, step, me, index).wait_recv()
            pl.when(second)(lambda: remote(2, step, me, index).wait_recv())

        @pl.when(second)
        def _():
            attend_block(rows, index, width_b, (0, width_b, None), main, tail, gate_rows, mixed)

        @pl.when(jnp.logical_not(second))
        def _():
            attend_block(
                rows, index, width_a, (0, width_a, 2 * width_a), main, tail, gate_rows, mixed
            )

        pl.when(me != index)(lambda: back_copy(index, me).start())
        pl.when(me == index)(lambda: back_own().start())

    for step in range(1, count):
        dest = lax.rem(me + step, count)
        remote(0, step, dest, me).wait_send()
        remote(1, step, dest, me).wait_send()
        pl.when(lax.rem(dest, 2) == 1)(lambda: remote(2, step, dest, me).wait_send())
        back_copy(dest, me).wait_send()
        back_copy(me, dest).wait_recv()
    back_own().wait()


def headwise_attention(
    query_a, key_a, value_a, query_b, key_b, value_b, cum_gates
):
    rows = query_a.shape[0]
    heads = cum_gates.shape[2]
    width_a = query_a.shape[1] // heads
    width_b = query_b.shape[1] // heads
    count = lax.axis_size("sp")

    def split(values, width):
        return values.reshape(rows, heads, width).transpose(1, 0, 2)

    pad = jnp.zeros((heads, rows, 2 * width_b - 3 * width_a), jnp.bfloat16)
    first = jnp.concatenate(
        [split(query_a, width_a), split(key_a, width_a), split(value_a, width_a), pad], axis=2
    )
    second = jnp.concatenate([split(query_b, width_b), split(key_b, width_b)], axis=2)
    packed = jnp.stack([first, second], axis=1).reshape(count, rows, 2 * width_b)
    late = split(value_b, width_b)
    gates = cum_gates.transpose(2, 1, 0).reshape(count, 1, rows)
    gates = jnp.broadcast_to(gates, (count, 8, rows))
    back = pl.pallas_call(
        functools.partial(attend_kernel, count, rows, width_a, width_b),
        out_shape=jax.ShapeDtypeStruct((count, rows, width_b), jnp.bfloat16),
        in_specs=[pl.BlockSpec(memory_space=pltpu.VMEM)] * 3,
        out_specs=pl.BlockSpec(memory_space=pltpu.VMEM),
        scratch_shapes=[
            pltpu.VMEM((count * rows, 2 * width_b), jnp.bfloat16),
            pltpu.VMEM((count * rows, width_b), jnp.bfloat16),
            pltpu.VMEM((8, count * rows), jnp.float32),
            pltpu.VMEM((count * rows, width_b), jnp.bfloat16),
            pltpu.SemaphoreType.DMA((3, count)),
            pltpu.SemaphoreType.DMA((3, count)),
            pltpu.SemaphoreType.DMA((3,)),
            pltpu.SemaphoreType.DMA((count,)),
            pltpu.SemaphoreType.DMA((count,)),
        ],
        compiler_params=pltpu.CompilerParams(collective_id=1, has_side_effects=True),
    )(packed, late, gates)
    attn_a = back[0::2, :, :width_a].transpose(1, 0, 2).reshape(rows, heads * width_a)
    attn_b = back[1::2].transpose(1, 0, 2).reshape(rows, heads * width_b)
    return attn_a, attn_b


def experts_kernel(
    count, narrow, parts, outgoing, w_gate, w_up, w_down, returned,
    gate_buf, up_buf, down_buf, piece, partial, taken, summed,
    weight_sem, out_sent, out_landed, own_sem, fan_sent, fan_landed,
    sum_sent, sum_landed, ret_sent, ret_landed,
):
    me = lax.axis_index("sp")
    mine = lax.axis_index("tp")
    _, slots, columns = outgoing.shape
    weights = [
        pltpu.make_async_copy(source, target, weight_sem.at[k])
        for k, (source, target) in enumerate(
            ((w_gate, gate_buf), (w_up, up_buf), (w_down, down_buf))
        )
    ]
    for copy in weights:
        copy.start()
    greet([("sp", count), ("tp", narrow)])

    def cols(index):
        return pl.ds(pl.multiple_of(index * columns, columns), columns)

    def step_rows(step):
        return pl.ds(pl.multiple_of(step * slots, slots), slots)

    def dispatch(step):
        peer = lax.rem(me + step, count)
        return send(
            outgoing.at[peer], piece.at[step_rows(step), cols(mine)],
            out_sent.at[step], out_landed.at[step], "sp", peer,
        )

    def fan(step, hop, owner):
        place = piece.at[step_rows(step), cols(owner)]
        return send(
            place, place, fan_sent.at[step, hop], fan_landed.at[step, hop],
            "tp", lax.rem(mine + hop, narrow),
        )

    for step in range(1, count):
        dispatch(step).start()
    own = pltpu.make_async_copy(
        outgoing.at[me], piece.at[step_rows(0), cols(mine)], own_sem.at[0]
    )
    own.start()
    for step in range(count):
        if step:
            dispatch(step).wait_recv()
        else:
            own.wait()
        for hop in range(1, narrow):
            fan(step, hop, mine).start()

    for copy in weights:
        copy.wait()
    steps = count // parts
    height = steps * slots

    def part_rows(part):
        return pl.ds(pl.multiple_of(part * height, height), height)

    def give(part, hop):
        peer = lax.rem(mine + hop, narrow)
        return send(
            partial.at[part_rows(part), cols(peer)], taken.at[hop - 1, part_rows(part), :],
            sum_sent.at[part, hop], sum_landed.at[part, hop], "tp", peer,
        )

    def compute(part, carry):
        for inner in range(steps):
            for hop in range(1, narrow):
                fan(part * steps + inner, hop, lax.rem(mine + narrow - hop, narrow)).wait_recv()
        rows = piece[part_rows(part), :]
        gate = jnp.dot(rows, gate_buf[...], preferred_element_type=jnp.float32)
        upward = jnp.dot(rows, up_buf[...], preferred_element_type=jnp.float32)
        hidden = (gate / (1.0 + jnp.exp(-gate)) * upward).astype(jnp.bfloat16)
        partial[part_rows(part), :] = jnp.dot(
            hidden, down_buf[...], preferred_element_type=jnp.float32
        ).astype(jnp.bfloat16)
        for hop in range(1, narrow):
            give(part, hop).start()
        return carry

    lax.fori_loop(0, parts, compute, 0)

    def give_back(step):
        peer = lax.rem(me + count - step, count)
        return send(
            summed.at[step_rows(step), :], returned.at[me],
            ret_sent.at[step], ret_landed.at[step], "sp", peer,
        )

    def returned_here(step):
        sender = lax.rem(me + step, count)
        return send(
            summed.at[step_rows(step), :], returned.at[sender],
            ret_sent.at[step], ret_landed.at[step], "sp", sender,
        )

    own_back = pltpu.make_async_copy(
        summed.at[step_rows(0), :], returned.at[me], own_sem.at[1]
    )
    for part in range(parts):
        here = slice(part * height, (part + 1) * height)
        total = partial[here, cols(mine)].astype(jnp.float32)
        for hop in range(1, narrow):
            give(part, hop).wait_recv()
            total = total + taken[hop - 1, here, :].astype(jnp.float32)
        summed[here, :] = total.astype(jnp.bfloat16)
        for inner in range(steps):
            step = part * steps + inner
            if step:
                give_back(step).start()
            else:
                own_back.start()
    for step in range(1, count):
        returned_here(step).wait_recv()
        give_back(step).wait_send()
        dispatch(step).wait_send()
    own_back.wait()
    for hop in range(1, narrow):
        for step in range(count):
            fan(step, hop, mine).wait_send()
        for part in range(parts):
            give(part, hop).wait_send()


def run_experts(outgoing, w_gate, w_up, w_down, parts):
    count, slots, columns = outgoing.shape
    narrow = lax.axis_size("tp")
    total = count * slots
    vmem = pl.BlockSpec(memory_space=pltpu.VMEM)
    hbm = pl.BlockSpec(memory_space=pl.ANY)
    dma = pltpu.SemaphoreType.DMA
    return pl.pallas_call(
        functools.partial(experts_kernel, count, narrow, parts),
        out_shape=jax.ShapeDtypeStruct(outgoing.shape, jnp.bfloat16),
        in_specs=[vmem, hbm, hbm, hbm],
        out_specs=vmem,
        scratch_shapes=[
            pltpu.VMEM(w_gate.shape, jnp.bfloat16),
            pltpu.VMEM(w_up.shape, jnp.bfloat16),
            pltpu.VMEM(w_down.shape, jnp.bfloat16),
            pltpu.VMEM((total, columns * narrow), jnp.bfloat16),
            pltpu.VMEM((total, columns * narrow), jnp.bfloat16),
            pltpu.VMEM((narrow - 1, total, columns), jnp.bfloat16),
            pltpu.VMEM((total, columns), jnp.bfloat16),
            dma((3,)),
            dma((count,)),
            dma((count,)),
            dma((2,)),
            dma((count, narrow)),
            dma((count, narrow)),
            dma((parts, narrow)),
            dma((parts, narrow)),
            dma((count,)),
            dma((count,)),
        ],
        compiler_params=pltpu.CompilerParams(collective_id=5, has_side_effects=True),
    )(outgoing, w_gate, w_up, w_down)


def gathered_attention(
    query_a, key_a, value_a, query_b, key_b, value_b, cum_gates
):
    rows = query_a.shape[0]
    heads = cum_gates.shape[2]
    width_a = query_a.shape[1] // heads
    width_b = query_b.shape[1] // heads
    here = lax.axis_index("sp")
    offset = here * rows
    gates_all = lax.all_gather(cum_gates, "sp", axis=0, tiled=True)
    queries_a = query_a.reshape(rows, heads, width_a)
    queries_b = query_b.reshape(rows, heads, width_b)
    blocks = [(queries_a, queries_b, offset + jnp.arange(rows, dtype=jnp.int32), cum_gates)]
    initial = tuple(
        (
            (
                empty_state(block[2].shape[0], heads, width_a),
                empty_state(block[2].shape[0], heads, width_b),
            )
            for block in blocks
        )
    )
    start = jnp.int32(0)
    piece_key_a = lax.all_gather(key_a.reshape(rows, heads, width_a), "sp", axis=0, tiled=True)
    piece_value_a = lax.all_gather(value_a.reshape(rows, heads, width_a), "sp", axis=0, tiled=True)
    piece_key_b = lax.all_gather(key_b.reshape(rows, heads, width_b), "sp", axis=0, tiled=True)
    piece_value_b = lax.all_gather(value_b.reshape(rows, heads, width_b), "sp", axis=0, tiled=True)
    item_count = piece_key_a.shape[0]
    key_pos = jnp.arange(item_count, dtype=jnp.int32)
    updated = []
    for state, (block_a, block_b, position, block_gate) in zip(initial, blocks):

        def compute(current):
            mask = key_pos[None, :] <= position[:, None]
            return (
                update_state(
                    current[0],
                    block_a,
                    piece_key_a,
                    piece_value_a,
                    block_gate[:, 0, :],
                    gates_all[:, 0, :],
                    mask,
                    width_a,
                ),
                update_state(
                    current[1],
                    block_b,
                    piece_key_b,
                    piece_value_b,
                    block_gate[:, 1, :],
                    gates_all[:, 1, :],
                    mask,
                    width_b,
                ),
            )

        updated.append(lax.cond(start <= position[-1], compute, lambda current: current, state))
    folded = tuple(updated)
    attn_a = finish(folded[0][0])
    attn_b = finish(folded[0][1])
    return attn_a, attn_b


def per_device(
    residual_in,
    query_a,
    key_a,
    value_a,
    query_b,
    key_b,
    value_b,
    cum_gates,
    out_a,
    out_b,
    post_gain,
    pre_gain,
    expert_ids,
    expert_weights,
    w_gate,
    w_up,
    w_down,
):
    rows = query_a.shape[0]
    heads = cum_gates.shape[2]
    width_a = query_a.shape[1] // heads
    width_b = query_b.shape[1] // heads
    group_size = lax.axis_size("sp")
    narrow = lax.axis_size("tp")
    columns = out_a.shape[1] // narrow
    own_rows = rows // narrow
    fits = 2 * heads == group_size and 2 * width_b >= 3 * width_a and width_b >= width_a
    attention = headwise_attention if fits else gathered_attention
    attn_a, attn_b = attention(query_a, key_a, value_a, query_b, key_b, value_b, cum_gates)
    part = (
        jnp.dot(attn_a, out_a, preferred_element_type=jnp.float32)
        + jnp.dot(attn_b, out_b, preferred_element_type=jnp.float32)
    ).astype(jnp.bfloat16)
    (parts,) = exchange(
        [part],
        [(narrow, own_rows, part.shape[1])],
        [(row_block(own_rows), item, 0)],
        "tp",
        3,
    )
    proj = jnp.sum(parts.astype(jnp.float32), axis=0).astype(jnp.bfloat16)
    post = rms_scale(proj.astype(jnp.float32), post_gain.astype(jnp.float32))
    mid_stream = (residual_in.astype(jnp.float32) + post).astype(jnp.bfloat16)
    normed = rms_scale(mid_stream.astype(jnp.float32), pre_gain.astype(jnp.float32)).astype(
        jnp.bfloat16
    )
    selected_count = expert_ids.shape[1]
    slots = rows * selected_count * 5 // (4 * group_size)
    named = expert_ids[:, :, None] == jnp.arange(group_size, dtype=jnp.int32)
    position = jnp.arange(rows, dtype=jnp.int32)
    before = (position[None, :] < position[:, None]).astype(jnp.bfloat16)
    earlier = jnp.dot(
        before, jnp.any(named, axis=1).astype(jnp.bfloat16), preferred_element_type=jnp.float32
    ).astype(jnp.int32)
    rank = jnp.sum(jnp.where(named, earlier[:, None, :], 0), axis=2)
    target = expert_ids * slots + rank
    chosen = target[:, :, None] == jnp.arange(group_size * slots, dtype=jnp.int32)
    weighting = jnp.sum(jnp.where(chosen, expert_weights[:, :, None], 0.0), axis=1)
    placing = jnp.any(chosen, axis=1).astype(jnp.bfloat16)
    (column_rows,) = exchange(
        [normed],
        [(rows, columns)],
        [(column_block(columns), row_block(own_rows), 0)],
        "tp",
        4,
    )
    outgoing = lax.dot_general(
        placing, column_rows, (((0,), (0,)), ((), ())), preferred_element_type=jnp.float32
    ).astype(jnp.bfloat16)
    outgoing = outgoing.reshape(group_size, slots, columns)
    if slots % 16 == 0 and group_size % 4 == 0:
        returned = run_experts(outgoing, w_gate[0], w_up[0], w_down[0], 4)
    else:
        (arrived,) = exchange(
            [outgoing], [(group_size, slots, columns)], [(item, item, 0)], "sp", 10
        )
        (piece,) = exchange(
            [arrived.reshape(-1, columns)],
            [(group_size * slots, columns * narrow)],
            [(whole_ref, column_block(columns), 0)],
            "tp",
            6,
        )
        gate = jnp.dot(piece, w_gate[0], preferred_element_type=jnp.float32)
        upward = jnp.dot(piece, w_up[0], preferred_element_type=jnp.float32)
        hidden = (jax.nn.silu(gate) * upward).astype(jnp.bfloat16)
        down = jnp.dot(hidden, w_down[0], preferred_element_type=jnp.float32).astype(jnp.bfloat16)
        (downs,) = exchange(
            [down],
            [(narrow, group_size * slots, columns)],
            [(column_block(columns), item, 0)],
            "tp",
            7,
        )
        summed = jnp.sum(downs.astype(jnp.float32), axis=0).astype(jnp.bfloat16)
        (returned,) = exchange(
            [summed.reshape(group_size, slots, columns)],
            [(group_size, slots, columns)],
            [(item, item, 0)],
            "sp",
            8,
        )
    mixture_cols = jnp.dot(
        weighting,
        returned.reshape(group_size * slots, columns).astype(jnp.float32),
        precision=lax.Precision.HIGHEST,
    )
    (mixture,) = exchange(
        [mixture_cols.astype(jnp.bfloat16)],
        [(own_rows, columns * narrow)],
        [(row_block(own_rows), column_block(columns), 0)],
        "tp",
        9,
    )
    return (mid_stream.astype(jnp.float32) + mixture.astype(jnp.float32)).astype(jnp.bfloat16)


def solution(mesh):
    placed = (
        P(("sp", "tp"), None),
        P("sp", "tp"),
        P("sp", "tp"),
        P("sp", "tp"),
        P("sp", "tp"),
        P("sp", "tp"),
        P("sp", "tp"),
        P("sp", None, "tp"),
        P("tp", None),
        P("tp", None),
        P(),
        P(),
        P("sp", None),
        P("sp", None),
        P("sp", None, "tp"),
        P("sp", None, "tp"),
        P("sp", "tp", None),
    )
    return jax.shard_map(
        per_device, mesh=mesh, in_specs=placed, out_specs=P(("sp", "tp"), None), check_vma=False
    )
```
